32 devices in a mesh: ep: 8 (over z, x), tp: 4 (over y, core).
Axes of the slice: x: 2, y: 2, z: 4, core: 2. Of those that a mesh axis runs over, the one named last changes fastest.
Arguments:
- query_rows: bfloat16 [3072, 4096], P('ep', 'tp'), may hold values from -6 to 6
- key_rows: bfloat16 [3072, 2048], P('ep', 'tp'), may hold values from -6 to 6
- value_rows: bfloat16 [3072, 2048], P('ep', 'tp'), may hold values from -6 to 6
- query_gain: float32 [128], replicated, may hold values from 0.4 to 5
- key_gain: float32 [128], replicated, may hold values from 0.4 to 5
- w_out: bfloat16 [4096, 2048], P('tp'), may hold values from -0.09375 to 0.09375
- mixer_gain: float32 [2048], replicated, may hold values from 0.1 to 1.9
- expert_input: bfloat16 [1536, 2048], P('ep'), may hold values from -6 to 6
- expert_ids: int32 [1536, 2], P('ep'), may hold values from 0 to 7, as said below
- expert_weights: float32 [1536, 2], P('ep'), may hold values from 0.1 to 1
- input_gain: float32 [2048], replicated, may hold values from 0.1 to 1.9
- w_gate: bfloat16 [8, 2048, 4096], P('ep', None, 'tp'), may hold values from -0.125 to 0.125
- w_up: bfloat16 [8, 2048, 4096], P('ep', None, 'tp'), may hold values from -0.125 to 0.125
- w_down: bfloat16 [8, 4096, 2048], P('ep', 'tp'), may hold values from -2 to 2
- out_gain: float32 [2048], P('tp'), may hold values from 0.1 to 1.9
Outputs:
- mixer_result: bfloat16 [3072, 2048], P(('ep', 'tp'))
- moe_result: bfloat16 [1536, 2048], P('ep', 'tp')
The draws below stay inside these ranges and needn't reach their ends.
Inputs may be any that keep to these rules, and one draw needn't show every extreme that they name: `expert_ids`: the two experts of a row differ and lie in one group of 2 consecutive experts. Among the rows of one index of ep (aligned blocks of 192 rows) no expert is named by more than 72 rows, and in every block some expert is named by exactly 72 rows.
All inputs are finite; a program needn't handle non-finite values.
Results may differ from the reference program's by a relative error of at most 0.02.
The reference program's roundings to bfloat16 on the way count: a program that leaves them out, or rounds other values in their place, can miss the bound.
Values may be sent and summed in bfloat16 or wider, within the bound.
A program may use at most 64 MiB of HBM per device.

```python
import math
import jax
import jax.numpy as jnp
from jax import lax

D = 2048
HEADS = 32
KV_HEADS = 16
HEAD = 128
GRID = 64
FF = 4096
GROUPS = 4
TOP = 2
ROWS2 = 192
EXPERTS = 8
INNER = 2
CAP = 72
TOK1 = 3072
TOK2 = 1536
N_EP = 8
N_TP = 4


def key_field(key):
    normal_base = jax.random.normal(jax.random.fold_in(key, 11), (TOK1, KV_HEADS * HEAD), jnp.float32)
    return jnp.clip(normal_base, -6.0, 6.0)


def draw_key_rows(key, part):
    return key_field(key).astype(jnp.bfloat16)


def draw_query_rows(key, part):
    fresh = jax.random.normal(jax.random.fold_in(key, 12), (TOK1, HEADS * HEAD), jnp.float32)
    return jnp.clip(fresh, -6.0, 6.0).astype(jnp.bfloat16)


def gain_field(key, offset):
    return jax.random.uniform(jax.random.fold_in(key, offset), (HEAD,), jnp.float32, 0.4, 1.6)


def draw_query_gain(key, part):
    return gain_field(key, 31)


def draw_key_gain(key, part):
    return gain_field(key, 32)


def draw_w_down(key, part):
    normal_base = jax.random.normal(jax.random.fold_in(key, 21), (EXPERTS, FF, D), jnp.float32) * FF ** (-0.5)
    column_ramp = jnp.exp(2.3 * jnp.arange(D, dtype=jnp.float32) / D)
    jitter = jax.random.uniform(jax.random.fold_in(key, 22), (D,), jnp.float32, 0.5, 1.5)
    return jnp.clip(normal_base * column_ramp * jitter, -2.0, 2.0).astype(jnp.bfloat16)


def block_ids(block_key):
    eighth = ROWS2 // 8
    shares = jnp.array([1, 2, 2, 3], jnp.int32)[jax.random.permutation(jax.random.fold_in(block_key, 1), 4)]
    group_sizes = shares * eighth
    group_ends = jnp.cumsum(group_sizes)
    starts = group_ends - group_sizes
    row_order = jnp.arange(ROWS2, dtype=jnp.int32)
    group_of = jnp.sum((row_order[:, None] >= group_ends[None, :]).astype(jnp.int32), axis=1)
    within = row_order - starts[group_of]
    shifts = jax.random.randint(jax.random.fold_in(block_key, 2), (GROUPS,), 1, INNER)
    labels = jax.vmap(lambda offset: jax.random.permutation(jax.random.fold_in(block_key, offset), INNER))(jnp.arange(GROUPS) + 3)
    first_pick = labels[group_of, within % INNER]
    second_pick = labels[group_of, (within + shifts[group_of]) % INNER]
    chosen_ids = jnp.stack([first_pick, second_pick], axis=1) + INNER * group_of[:, None]
    shuffle = jax.random.permutation(jax.random.fold_in(block_key, 9), ROWS2)
    return chosen_ids[shuffle].astype(jnp.int32)


def draw_expert_ids(key, part):
    block_keys = jax.vmap(lambda block_index: jax.random.fold_in(key, block_index))(jnp.arange(N_EP) + 100)
    return jax.vmap(block_ids)(block_keys).reshape(TOK2, TOP)


def shard_levels(own_key, dims, shards, smallest, top_value):
    loudness, own = 1.0, jax.random.fold_in(own_key, 6)
    for dim, parts in shards:
        steps = jnp.exp(jax.random.uniform(jax.random.fold_in(own, dim), (parts,), jnp.float32, smallest / len(shards), top_value / len(shards)))
        loudness = loudness * jnp.repeat(steps, dims[dim] // parts).reshape([-1 if axis == dim else 1 for axis in range(len(dims))])
    return loudness


def scatter_about(rng, dims, width, reach, pieces=(), held_as=jnp.bfloat16):
    level = shard_levels(rng, dims, pieces, -0.22, 0.18) if pieces else 1.0
    drawn = jax.random.normal(rng, dims, jnp.float32) * width * level
    return jnp.minimum(jnp.maximum(drawn, -reach), reach).astype(held_as)


def setup_inputs(seed: int = 0) -> dict:
    key_list = jax.random.split(jax.random.key(seed), 16)
    query_rows = draw_query_rows(jax.random.fold_in(key_list[15], 71), 0)
    key_rows = draw_key_rows(jax.random.fold_in(key_list[15], 71), 0)
    value_rows = scatter_about(key_list[2], (TOK1, KV_HEADS * HEAD), 1.0, 6.0, ((0, 8), (1, 4)))
    query_gain = draw_query_gain(jax.random.fold_in(key_list[15], 71), 0)
    key_gain = draw_key_gain(jax.random.fold_in(key_list[15], 71), 0)
    w_out = scatter_about(key_list[5], (HEADS * HEAD, D), (HEADS * HEAD) ** -0.5, 0.09375, ((0, 4),))
    mixer_gain = jnp.clip(1.0 + 0.18 * jax.random.normal(key_list[6], (D,), jnp.float32), 0.1, 1.9)
    expert_input = scatter_about(key_list[7], (TOK2, D), 1.0, 6.0, ((0, 8),))
    expert_ids = draw_expert_ids(jax.random.fold_in(key_list[15], 71), 0)
    expert_weights = jnp.clip(jnp.exp(math.log(1.0) - 2.3025851 * jax.random.uniform(key_list[9], (TOK2, TOP), jnp.float32) ** shard_levels(key_list[9], (TOK2, TOP), ((0, 8),), -0.2, 0.2)), 0.1, 1.0)
    input_gain = jnp.clip(1.0 + 0.18 * jax.random.normal(key_list[10], (D,), jnp.float32), 0.1, 1.9)
    w_gate = scatter_about(key_list[11], (EXPERTS, D, FF), D ** -0.5, 0.125, ((0, 8), (2, 4)))
    w_up = scatter_about(key_list[12], (EXPERTS, D, FF), D ** -0.5, 0.125, ((0, 8), (2, 4)))
    w_down = draw_w_down(jax.random.fold_in(key_list[15], 71), 0)
    out_gain = jnp.clip(1.0 + 0.18 * jax.random.normal(key_list[14], (D,), jnp.float32), 0.1, 1.9)
    return {"query_rows": query_rows, "key_rows": key_rows, "value_rows": value_rows, "query_gain": query_gain, "key_gain": key_gain, "w_out": w_out, "mixer_gain": mixer_gain, "expert_input": expert_input, "expert_ids": expert_ids, "expert_weights": expert_weights, "input_gain": input_gain, "w_gate": w_gate, "w_up": w_up, "w_down": w_down, "out_gain": out_gain}


EPS = 1e-06
THETA = 10000.0

def turn_half(half_part, position):
    half_width = half_part.shape[-1]
    frequency = THETA ** (-jnp.arange(0, half_width, 2, dtype=jnp.float32) / half_width)
    angles = position[:, None, None] * frequency[None, None, :]
    cosine = jnp.cos(angles)
    sine_part = jnp.sin(angles)
    first_half = half_part[..., :half_width // 2]
    second = half_part[..., half_width // 2:]
    return jnp.concatenate([first_half * cosine - second * sine_part, second * cosine + first_half * sine_part], axis=-1)

def norm_turn(raw_rows, gain_vec, row_offset):
    row_count = raw_rows.shape[0]
    head_dim = gain_vec.shape[0]
    head_count = raw_rows.shape[1] // head_dim
    by_head = raw_rows.astype(jnp.float32).reshape(row_count, head_count, head_dim)
    scaled = by_head * lax.rsqrt(lax.optimization_barrier(jnp.mean(by_head * by_head, axis=-1, keepdims=True)) + EPS) * gain_vec
    position = row_offset + jnp.arange(row_count, dtype=jnp.int32)
    grid_row = (position // GRID).astype(jnp.float32)
    grid_col = (position % GRID).astype(jnp.float32)
    half_dim = head_dim // 2
    turned = jnp.concatenate([turn_half(scaled[..., :half_dim], grid_row), turn_half(scaled[..., half_dim:], grid_col)], axis=-1)
    return turned.reshape(row_count, head_count * head_dim).astype(jnp.bfloat16)

def mixer_ref(query_rows, key_rows, value_rows, query_gain, key_gain, w_out, mixer_gain):
    token_count = query_rows.shape[0]
    group_size = HEADS // KV_HEADS
    query_turned = norm_turn(query_rows, query_gain, 0)
    key_turned = norm_turn(key_rows, key_gain, 0)
    query_heads = query_turned.reshape(token_count, HEADS, HEAD).transpose(1, 0, 2)
    key_heads = jnp.repeat(key_turned.reshape(token_count, KV_HEADS, HEAD).transpose(1, 0, 2), group_size, axis=0)
    value_heads = jnp.repeat(value_rows.reshape(token_count, KV_HEADS, HEAD).transpose(1, 0, 2), group_size, axis=0)

    def one_head(head_triple):
        query_head, key_head, value_head = head_triple
        scores = jnp.dot(query_head, key_head.T, preferred_element_type=jnp.float32) * HEAD ** (-0.5)
        row_max = lax.optimization_barrier(jnp.max(scores, axis=1, keepdims=True))
        exponent = jnp.exp(scores - row_max)
        probs = exponent.astype(jnp.bfloat16)
        numer = jnp.dot(probs, value_head, preferred_element_type=jnp.float32)
        return (numer / lax.optimization_barrier(jnp.sum(exponent, axis=1, keepdims=True))).astype(jnp.bfloat16)
    attended = lax.map(one_head, (query_heads, key_heads, value_heads))
    attended = attended.transpose(1, 0, 2).reshape(token_count, HEADS * HEAD)
    block_width = HEADS * HEAD // N_TP
    attended_blocks = attended.reshape(token_count, N_TP, block_width).transpose(1, 0, 2)
    weight_blocks = w_out.reshape(N_TP, block_width, D)

    def add_part(running_sum, block_pair):
        attended_block, weight_block = block_pair
        head_part = jnp.dot(attended_block, weight_block, preferred_element_type=jnp.float32).astype(jnp.bfloat16)
        head_part = lax.optimization_barrier(head_part)
        return (running_sum + head_part.astype(jnp.float32), None)
    mixed_sum, _ = lax.scan(add_part, jnp.zeros((token_count, D), jnp.float32), (attended_blocks, weight_blocks))
    scaled = mixed_sum * lax.rsqrt(lax.optimization_barrier(jnp.mean(mixed_sum * mixed_sum, axis=1, keepdims=True)) + EPS) * mixer_gain
    return scaled.astype(jnp.bfloat16)

def expert_ref(expert_input, expert_ids, expert_weights, input_gain, w_gate, w_up, w_down, out_gain):
    token_count = expert_input.shape[0]
    inputs_f = expert_input.astype(jnp.float32)
    normed = (inputs_f * lax.rsqrt(lax.optimization_barrier(jnp.mean(inputs_f * inputs_f, axis=1, keepdims=True)) + EPS) * input_gain).astype(jnp.bfloat16)
    padded = jnp.concatenate([normed, jnp.zeros((1, D), jnp.bfloat16)], axis=0)
    flat_ids = expert_ids.reshape(-1)
    pick_count = flat_ids.shape[0]
    top_count = expert_ids.shape[1]
    weight_flat = jnp.concatenate([expert_weights.reshape(-1), jnp.zeros((1,), jnp.float32)])
    slot_total = N_EP * CAP
    block_width = FF // N_TP

    def one_expert(accum, expert_index):
        chosen = flat_ids == expert_index
        position = jnp.cumsum(chosen.astype(jnp.int32)) - 1
        target = jnp.where(chosen, position, slot_total).astype(jnp.int32)
        pick_table = jnp.full((slot_total,), pick_count, jnp.int32).at[target].set(jnp.arange(pick_count, dtype=jnp.int32), mode='drop')
        token_table = (pick_table // top_count).astype(jnp.int32)
        gathered = jnp.take(padded, token_table, axis=0)
        gate_weight = lax.dynamic_index_in_dim(w_gate, expert_index, 0, keepdims=False)
        up_weight = lax.dynamic_index_in_dim(w_up, expert_index, 0, keepdims=False)
        down_weight = lax.dynamic_index_in_dim(w_down, expert_index, 0, keepdims=False)
        gate_pre = jnp.dot(gathered, gate_weight, preferred_element_type=jnp.float32)
        up_pre = jnp.dot(gathered, up_weight, preferred_element_type=jnp.float32)
        hidden = (jax.nn.silu(gate_pre) * up_pre).astype(jnp.bfloat16)
        hidden_blocks = hidden.reshape(slot_total, N_TP, block_width).transpose(1, 0, 2).astype(jnp.float32)
        down_blocks = down_weight.reshape(N_TP, block_width, D).astype(jnp.float32)
        expert_part = jnp.einsum('jsf,jfd->jsd', hidden_blocks, down_blocks).astype(jnp.bfloat16)
        expert_part = lax.optimization_barrier(expert_part)
        expert_rows = lax.optimization_barrier(jnp.sum(expert_part.astype(jnp.float32), axis=0)).astype(jnp.bfloat16)
        weights_now = jnp.take(weight_flat, pick_table)
        accum = accum.at[token_table].add(weights_now[:, None] * expert_rows.astype(jnp.float32), mode='drop')
        return (accum, None)
    combined, _ = lax.scan(one_expert, jnp.zeros((token_count, D), jnp.float32), jnp.arange(EXPERTS, dtype=jnp.int32))
    scaled = combined * lax.rsqrt(lax.optimization_barrier(jnp.mean(combined * combined, axis=1, keepdims=True)) + EPS) * out_gain
    return scaled.astype(jnp.bfloat16)

def reference(query_rows, key_rows, value_rows, query_gain, key_gain, w_out, mixer_gain, expert_input, expert_ids, expert_weights, input_gain, w_gate, w_up, w_down, out_gain):
    mixer_result = mixer_ref(query_rows, key_rows, value_rows, query_gain, key_gain, w_out, mixer_gain)
    moe_result = expert_ref(expert_input, expert_ids, expert_weights, input_gain, w_gate, w_up, w_down, out_gain)
    return (mixer_result, moe_result)
```

```python
import functools
import math

import jax
import jax.numpy as jnp
from jax import lax
from jax.experimental import pallas as pl
from jax.experimental.pallas import tpu as pltpu
from jax.sharding import PartitionSpec as P

D = 2048
GRID = 64
GROUPS = 4
BLOCK_Q = 384
BLOCK_K = 768


EPS = 1e-06
THETA = 10000.0


def turn_half(half_part, position):
    half_width = half_part.shape[-1]
    frequency = THETA ** (-jnp.arange(0, half_width, 2, dtype=jnp.float32) / half_width)
    angles = position[:, None, None] * frequency[None, None, :]
    cosine = jnp.cos(angles)
    sine_part = jnp.sin(angles)
    first_half = half_part[..., : half_width // 2]
    second = half_part[..., half_width // 2 :]
    return jnp.concatenate(
        [first_half * cosine - second * sine_part, second * cosine + first_half * sine_part],
        axis=-1,
    )


def norm_turn(raw_rows, gain_vec, row_offset):
    row_count = raw_rows.shape[0]
    head_dim = gain_vec.shape[0]
    head_count = raw_rows.shape[1] // head_dim
    by_head = raw_rows.astype(jnp.float32).reshape(row_count, head_count, head_dim)
    scaled = (
        by_head * lax.rsqrt(jnp.mean(by_head * by_head, axis=-1, keepdims=True) + EPS) * gain_vec
    )
    position = row_offset + jnp.arange(row_count, dtype=jnp.int32)
    grid_row = (position // GRID).astype(jnp.float32)
    grid_col = (position % GRID).astype(jnp.float32)
    half_dim = head_dim // 2
    turned = jnp.concatenate(
        [turn_half(scaled[..., :half_dim], grid_row), turn_half(scaled[..., half_dim:], grid_col)],
        axis=-1,
    )
    return turned.reshape(row_count, head_count * head_dim).astype(jnp.bfloat16)


def attend_kernel(scale, block_keys, q_ref, k_ref, v_ref, o_ref, vt_ref):
    @pl.when(pl.program_id(1) == 0)
    def _():
        vt_ref[...] = v_ref[...].T

    query = q_ref[...]
    columns = query.shape[0]
    head_dim = query.shape[1]
    steps = k_ref.shape[0] // block_keys

    def step(index, carry):
        top, total, acc = carry
        rows = pl.ds(pl.multiple_of(index * block_keys, block_keys), block_keys)
        scores = (
            lax.dot_general(
                k_ref[rows, :],
                query,
                (((1,), (1,)), ((), ())),
                preferred_element_type=jnp.float32,
            )
            * scale
        )
        new_top = jnp.maximum(top, jnp.max(scores, axis=0, keepdims=True))
        exponent = jnp.exp2(scores - new_top)
        factor = jnp.exp2(top - new_top)
        total = total * factor + jnp.sum(exponent, axis=0, keepdims=True)
        acc = acc * factor + jnp.dot(
            vt_ref[:, rows], exponent.astype(jnp.bfloat16), preferred_element_type=jnp.float32
        )
        return new_top, total, acc

    carry = (
        jnp.full((1, columns), -1e30, jnp.float32),
        jnp.zeros((1, columns), jnp.float32),
        jnp.zeros((head_dim, columns), jnp.float32),
    )
    if steps <= 8:
        for index in range(steps):
            carry = step(index, carry)
    else:
        carry = lax.fori_loop(0, steps, step, carry)
    _, total, acc = carry
    o_ref[...] = (acc / total).T.astype(o_ref.dtype)


def divisor(size, limit):
    block = limit
    while size % block:
        block -= 128
    return block


def attend(query, key, value, heads, head_dim, group_size, q_col, k_col, v_col):
    tokens = query.shape[0]
    keys = key.shape[0]
    block_q = divisor(tokens, BLOCK_Q)
    block_k = divisor(keys, BLOCK_K)
    flops = 4 * heads * tokens * keys * head_dim
    return pl.pallas_call(
        functools.partial(attend_kernel, head_dim**-0.5 * math.log2(math.e), block_k),
        grid=(heads, tokens // block_q),
        in_specs=[
            pl.BlockSpec((block_q, head_dim), lambda h, i: (i, q_col + h)),
            pl.BlockSpec((keys, head_dim), lambda h, i: (0, k_col + h // group_size)),
            pl.BlockSpec((keys, head_dim), lambda h, i: (0, v_col + h // group_size)),
        ],
        out_specs=pl.BlockSpec((block_q, head_dim), lambda h, i: (i, h)),
        out_shape=jax.ShapeDtypeStruct((tokens, heads * head_dim), jnp.bfloat16),
        scratch_shapes=[pltpu.VMEM((head_dim, keys), jnp.bfloat16)],
        compiler_params=pltpu.CompilerParams(dimension_semantics=("arbitrary", "arbitrary")),
        cost_estimate=pl.CostEstimate(
            flops=2 * flops,
            bytes_accessed=8 * tokens * heads * head_dim,
            transcendentals=heads * tokens * keys,
        ),
        name="attend",
    )(query, key, value)


def mixer_half(query_rows, key_rows, value_rows, query_gain, key_gain, w_out, mixer_gain):
    row_count = query_rows.shape[0]
    head_dim = query_gain.shape[0]
    n_ep = lax.axis_size("ep")
    row_offset = lax.axis_index("ep") * row_count
    query_turned = norm_turn(query_rows, query_gain, row_offset)
    key_turned = norm_turn(key_rows, key_gain, row_offset)
    local_heads = query_rows.shape[1] // head_dim
    group_size = query_rows.shape[1] // key_rows.shape[1]
    if local_heads == n_ep:
        by_head = [
            x.reshape(row_count, -1, head_dim).transpose(1, 0, 2)
            for x in (query_turned, key_turned, value_rows)
        ]
        outgoing = jnp.concatenate(
            [by_head[0]] + [jnp.repeat(x, group_size, axis=0) for x in by_head[1:]], axis=2
        )
        arrived = lax.all_to_all(outgoing, "ep", split_axis=0, concat_axis=0, tiled=True)
        packed = arrived.reshape(n_ep * row_count, 3 * head_dim)
        one_head = attend(packed, packed, packed, 1, head_dim, 1, 0, 1, 2)
        back = lax.all_to_all(
            one_head.reshape(n_ep, row_count, head_dim),
            "ep",
            split_axis=0,
            concat_axis=0,
            tiled=True,
        )
        attended = back.transpose(1, 0, 2).reshape(row_count, local_heads * head_dim)
    else:
        key_all = lax.all_gather(key_turned, "ep", axis=0, tiled=True)
        value_all = lax.all_gather(value_rows, "ep", axis=0, tiled=True)
        attended = attend(
            query_turned, key_all, value_all, local_heads, head_dim, group_size, 0, 0, 0
        )
    mixed_sum = lax.psum_scatter(
        jnp.dot(attended, w_out, preferred_element_type=jnp.float32).astype(jnp.bfloat16),
        "tp",
        scatter_dimension=0,
        tiled=True,
    ).astype(jnp.float32)
    scaled = (
        mixed_sum
        * lax.rsqrt(jnp.mean(mixed_sum * mixed_sum, axis=1, keepdims=True) + EPS)
        * mixer_gain
    )
    return scaled.astype(jnp.bfloat16)


def expert_half(
    expert_input, expert_ids, expert_weights, input_gain, w_gate, w_up, w_down, out_gain
):
    row_count, width = expert_input.shape
    top_count = expert_ids.shape[1]
    n_tp = lax.axis_size("tp")
    expert_total = w_gate.shape[0] * lax.axis_size("ep")
    inner_count = expert_total // GROUPS
    capacity = 3 * row_count // (4 * inner_count)
    slots = expert_total * capacity
    inputs_f = expert_input.astype(jnp.float32)
    normed = (
        inputs_f
        * lax.rsqrt(jnp.mean(inputs_f * inputs_f, axis=1, keepdims=True) + EPS)
        * input_gain
    ).astype(jnp.bfloat16)
    row_index = jnp.arange(row_count, dtype=jnp.int32)
    before = row_index[None, :] < row_index[:, None]
    slot_index = jnp.arange(slots, dtype=jnp.int32)
    slot_of = []
    for k in range(top_count):
        same = jnp.zeros((row_count, row_count), bool)
        for other in range(top_count):
            same = same | (expert_ids[:, k][:, None] == expert_ids[:, other][None, :])
        rank = jnp.sum((same & before).astype(jnp.int32), axis=1)
        slot_of.append(expert_ids[:, k] * capacity + rank)
    chosen = [slot_index[:, None] == slot[None, :] for slot in slot_of]
    picker = functools.reduce(jnp.logical_or, chosen).astype(jnp.bfloat16)
    share = width // n_tp
    own = lax.dynamic_slice_in_dim(normed, lax.axis_index("tp") * share, share, axis=1)
    outgoing = jnp.dot(picker, own, preferred_element_type=jnp.float32).astype(jnp.bfloat16)
    arrived = lax.all_to_all(
        outgoing.reshape(expert_total, capacity, share),
        "ep",
        split_axis=0,
        concat_axis=0,
        tiled=True,
    ).reshape(slots, share)
    shares = lax.all_gather(arrived, "tp", axis=0, tiled=False)
    arrived = jnp.concatenate([shares[j] for j in range(n_tp)], axis=1)
    gate_pre = jnp.dot(arrived, w_gate[0], preferred_element_type=jnp.float32)
    up_pre = jnp.dot(arrived, w_up[0], preferred_element_type=jnp.float32)
    hidden = (jax.nn.silu(gate_pre) * up_pre).astype(jnp.bfloat16)
    partial_term = jnp.dot(hidden, w_down[0], preferred_element_type=jnp.float32)
    summed = lax.psum_scatter(
        partial_term.astype(jnp.bfloat16), "tp", scatter_dimension=1, tiled=True
    )
    returned = lax.all_to_all(summed, "ep", split_axis=0, concat_axis=0, tiled=True)
    combined = jnp.zeros((row_count, returned.shape[1]), jnp.float32)
    for k in range(top_count):
        select = (slot_of[k][:, None] == slot_index[None, :]).astype(jnp.bfloat16)
        picked = jnp.dot(select, returned, preferred_element_type=jnp.float32)
        combined = combined + picked * expert_weights[:, k][:, None]
    squares = lax.psum(jnp.sum(combined * combined, axis=1), "tp")
    scaled = combined * lax.rsqrt(squares / D + EPS)[:, None] * out_gain
    return scaled.astype(jnp.bfloat16)


def per_device(
    query_rows,
    key_rows,
    value_rows,
    query_gain,
    key_gain,
    w_out,
    mixer_gain,
    expert_input,
    expert_ids,
    expert_weights,
    input_gain,
    w_gate,
    w_up,
    w_down,
    out_gain,
):
    mixer_result = mixer_half(
        query_rows, key_rows, value_rows, query_gain, key_gain, w_out, mixer_gain
    )
    moe_result = expert_half(
        expert_input, expert_ids, expert_weights, input_gain, w_gate, w_up, w_down, out_gain
    )
    return (mixer_result, moe_result)


def solution(mesh):
    return jax.shard_map(
        per_device,
        mesh=mesh,
        in_specs=(
            P("ep", "tp"),
            P("ep", "tp"),
            P("ep", "tp"),
            P(),
            P(),
            P("tp", None),
            P(),
            P("ep", None),
            P("ep", None),
            P("ep", None),
            P(),
            P("ep", None, "tp"),
            P("ep", None, "tp"),
            P("ep", "tp", None),
            P("tp"),
        ),
        out_specs=(P(("ep", "tp"), None), P("ep", "tp")),
        check_vma=False,
    )
```
